32 devices in a mesh: sp: 8 (over z, y), tp: 4 (over x, core).
Axes of the slice: x: 2, y: 2, z: 4, core: 2. Of those that a mesh axis runs over, the one named last changes fastest.
Arguments:
- out_grad: bfloat16 [1024, 2048], P('sp', 'tp'), may hold values from -6 to 6
- route_ids: int32 [1024, 2], P('sp'), may hold values from 0 to 7, as said below
- route_weight: float32 [1024, 2], P('sp'), may hold values from 0.1 to 0.9
- expert_inputs: bfloat16 [8, 512, 2048], P('sp'), may hold values from -6 to 6
- gate_weight: bfloat16 [8, 2048, 3072], P('sp', None, 'tp'), may hold values from -0.125 to 0.125
- up_weight: bfloat16 [8, 2048, 3072], P('sp', None, 'tp'), may hold values from -0.125 to 0.125
- down_weight: bfloat16 [8, 3072, 2048], P('sp', 'tp'), may hold values from -0.109375 to 0.109375
- out_gate: bfloat16 [1024, 2048], P('sp', 'tp'), may hold values from -6 to 6
- in_gate: bfloat16 [1024, 2048], P('sp', 'tp'), may hold values from -6 to 6
- values: bfloat16 [1024, 2048], P('sp', 'tp'), may hold values from -6 to 6
- conv_out: bfloat16 [1024, 2048], P('sp', 'tp'), may hold values from -6 to 6
- conv_taps: bfloat16 [3, 2048], P(None, 'tp'), may hold values from -3.5 to 3.5
- proj_weight: bfloat16 [2048, 2048], P(None, 'tp'), may hold values from -0.125 to 0.125
Outputs:
- resid_grad: bfloat16 [1024, 2048], P('sp', 'tp')
- out_gate_grad: bfloat16 [1024, 2048], P('sp', 'tp')
- in_gate_grad: bfloat16 [1024, 2048], P('sp', 'tp')
- values_grad: bfloat16 [1024, 2048], P('sp', 'tp')
- proj_grad: float32 [2048, 2048], P('sp', 'tp')
- gate_grad: bfloat16 [8, 2048, 3072], P('sp', None, 'tp')
- up_grad: bfloat16 [8, 2048, 3072], P('sp', None, 'tp')
- down_grad: bfloat16 [8, 3072, 2048], P('sp', 'tp')
The draws below stay inside these ranges and needn't reach their ends.
Inputs may be any that keep to these rules, and one draw needn't show every extreme that they name: `route_ids`: each row names two different experts. Among the rows of one device (aligned blocks of 128 rows) no expert is named more than 64 times, and in every draw one expert is named exactly 64 times in every block.
All inputs are finite; a program needn't handle non-finite values.
Results may differ from the reference program's by a relative error of at most 0.017.
Values may be sent and summed in bfloat16 or wider, within the bound.
No kernel may reach another device: no remote copies, remote signals or barrier semaphores. Data moves between devices by JAX's collectives and lax.ppermute only.
A program may use at most 128 MiB of HBM per device.

```python
import math
import jax
import jax.numpy as jnp
from jax import lax

D = 2048
FF = 3072
TAPS = 3
TOK_DEV = 128
TOKENS = 1024
EXPERTS = 8
CAP = 64
SLOTS = 512
N_TP = 4


def draw_route_ids(key, part):
    blocks = TOKENS // TOK_DEV
    tickets = jnp.arange(EXPERTS * CAP, dtype=jnp.int32) // CAP
    filled = jax.random.randint(jax.random.fold_in(key, 11), (), 0, EXPERTS)

    def one_block(block_key):
        extra = jax.random.randint(jax.random.fold_in(block_key, 1), (), 0, EXPERTS)
        shuffled = tickets[jax.random.permutation(jax.random.fold_in(block_key, 2), EXPERTS * CAP)]
        priority = jnp.where(shuffled == filled, 0, jnp.where(shuffled == extra, 1, 2)).astype(jnp.int32)
        chosen = shuffled[jnp.argsort(priority, stable=True)][:2 * TOK_DEV]
        ordered = jnp.sort(chosen)
        pairs = jnp.stack([ordered[:TOK_DEV], ordered[TOK_DEV:]], axis=1)
        flips = jax.random.randint(jax.random.fold_in(block_key, 3), (TOK_DEV, 1), 0, 2)
        pairs = jnp.where(flips == 1, pairs[:, ::-1], pairs)
        shuffle_rows = jax.random.permutation(jax.random.fold_in(block_key, 4), TOK_DEV)
        return pairs[shuffle_rows]
    block_keys = jax.random.split(jax.random.fold_in(key, 7), blocks)
    return jax.vmap(one_block)(block_keys).reshape(TOKENS, 2).astype(jnp.int32)


def spiked(values, key, source, target, blocks, factor):
    def block_of(position):
        return (jnp.arange(values.shape[position]) // (values.shape[position] // blocks)).reshape((-1,) + (1,) * (values.ndim - 1 - position))

    first = jax.random.permutation(key, blocks)[block_of(target)]
    other_side = (block_of(target) + blocks // 2) % blocks
    return jnp.where((block_of(source) == first) | (block_of(source) == other_side), factor * values, values)


def levels(rng, extent, pieces, least, largest):
    level, own = 1.0, jax.random.fold_in(rng, 6)
    for axis_at, parts in pieces:
        heights = jnp.exp(jax.random.uniform(jax.random.fold_in(own, axis_at), (parts,), jnp.float32, least / len(pieces), largest / len(pieces)))
        level = level * jnp.repeat(heights, extent[axis_at] // parts).reshape([-1 if axis == axis_at else 1 for axis in range(len(extent))])
    return level


def centred(own_key, dims, deviation, reach, cuts=(), held_as=jnp.bfloat16):
    level = levels(own_key, dims, cuts, -0.22, 0.18) if cuts else 1.0
    entries = jax.random.normal(own_key, dims, jnp.float32) * deviation * level
    return jnp.minimum(jnp.maximum(entries, -reach), reach).astype(held_as)


def bell_draw_with(own_key, shape, scale, bound, shards, heavy, kind=jnp.bfloat16):
    values = scale * jax.random.normal(own_key, shape, jnp.float32)
    if shards:
        values = values * levels(own_key, shape, shards, -0.22, 0.18)
    return jnp.clip(spiked(values, jax.random.fold_in(own_key, 3), *heavy), -bound, bound).astype(kind)


def setup_inputs(seed: int = 0) -> dict:
    streams_of = jax.random.split(jax.random.key(seed), 14)
    out_grad = bell_draw_with(streams_of[0], (TOKENS, D), 1.0, 6.0, ((0, 8), (1, 4)), (0, 1, 8, 2.0))
    route_ids = draw_route_ids(jax.random.fold_in(streams_of[13], 71), 0)
    route_weight = jnp.clip(0.1 + 0.79999997 * jax.random.uniform(streams_of[2], (TOKENS, 2), jnp.float32) ** levels(streams_of[2], (TOKENS, 2), ((0, 8),), -0.2, 0.2), 0.1, 0.9)
    expert_inputs = centred(streams_of[3], (EXPERTS, SLOTS, D), 1.0, 6.0, ((0, 8),))
    gate_weight = centred(streams_of[4], (EXPERTS, D, FF), D ** -0.5, 0.125, ((0, 8), (2, 4)))
    up_weight = centred(streams_of[5], (EXPERTS, D, FF), D ** -0.5, 0.125, ((0, 8), (2, 4)))
    down_weight = centred(streams_of[6], (EXPERTS, FF, D), FF ** -0.5, 0.109375, ((0, 8), (1, 4)))
    out_gate = centred(streams_of[7], (TOKENS, D), 1.0, 6.0, ((0, 8), (1, 4)))
    in_gate = centred(streams_of[8], (TOKENS, D), 1.0, 6.0, ((0, 8), (1, 4)))
    values = centred(streams_of[9], (TOKENS, D), 1.0, 6.0, ((0, 8), (1, 4)))
    conv_out = centred(streams_of[10], (TOKENS, D), 1.0, 6.0, ((0, 8), (1, 4)))
    conv_taps = centred(streams_of[11], (TAPS, D), TAPS ** -0.5, 3.5, ((1, 4),))
    proj_weight = centred(streams_of[12], (D, D), D ** -0.5, 0.125, ((1, 4),))
    return dict(out_grad=out_grad, route_ids=route_ids, route_weight=route_weight, expert_inputs=expert_inputs, gate_weight=gate_weight, up_weight=up_weight, down_weight=down_weight, out_gate=out_gate, in_gate=in_gate, values=values, conv_out=conv_out, conv_taps=conv_taps, proj_weight=proj_weight)


def slot_rows(route_ids):
    blocks = route_ids.reshape(TOKENS // TOK_DEV, 2 * TOK_DEV)
    onehot = (blocks[:, :, None] == jnp.arange(EXPERTS, dtype=jnp.int32)[None, None, :]).astype(jnp.int32)
    ranked = lax.optimization_barrier(jnp.sum((jnp.cumsum(onehot, axis=1) - onehot) * onehot, axis=2))
    source = jnp.arange(TOKENS // TOK_DEV, dtype=jnp.int32)[:, None]
    return (blocks * SLOTS + source * CAP + ranked).reshape(-1).astype(jnp.int32)

def expert_step(operands):
    inputs, routed, gate_w, up_w, down_w = operands
    pre_gate = jnp.dot(inputs, gate_w, preferred_element_type=jnp.float32)
    pre_up = jnp.dot(inputs, up_w, preferred_element_type=jnp.float32)
    sigmoid_g = jax.nn.sigmoid(pre_gate)
    activated = pre_gate * sigmoid_g
    hidden = (activated * pre_up).astype(jnp.bfloat16)
    d_hidden = jnp.dot(routed, down_w.T, preferred_element_type=jnp.float32)
    d_gate = (d_hidden * pre_up * sigmoid_g * (1.0 + pre_gate * (1.0 - sigmoid_g))).astype(jnp.bfloat16)
    d_up = (d_hidden * activated).astype(jnp.bfloat16)
    slot_scale = 1.0 / math.sqrt(SLOTS)
    gate_grad = (jnp.dot(inputs.T, d_gate, preferred_element_type=jnp.float32) * slot_scale).astype(jnp.bfloat16)
    up_grad = (jnp.dot(inputs.T, d_up, preferred_element_type=jnp.float32) * slot_scale).astype(jnp.bfloat16)
    down_grad = (jnp.dot(hidden.T, routed, preferred_element_type=jnp.float32) * slot_scale).astype(jnp.bfloat16)
    block_width = FF // N_TP
    back = jnp.zeros((SLOTS, D), jnp.float32)
    for block in range(N_TP):
        lower = block * block_width
        upper = lower + block_width
        part_sum = jnp.dot(lax.slice_in_dim(d_gate, lower, upper, axis=1), lax.slice_in_dim(gate_w, lower, upper, axis=1).T, preferred_element_type=jnp.float32)
        part_sum = part_sum + jnp.dot(lax.slice_in_dim(d_up, lower, upper, axis=1), lax.slice_in_dim(up_w, lower, upper, axis=1).T, preferred_element_type=jnp.float32)
        back = back + lax.optimization_barrier(part_sum.astype(jnp.bfloat16)).astype(jnp.float32)
    return (gate_grad, up_grad, down_grad, back.astype(jnp.bfloat16))

def reference(out_grad, route_ids, route_weight, expert_inputs, gate_weight, up_weight, down_weight, out_gate, in_gate, values, conv_out, conv_taps, proj_weight):
    rows = slot_rows(route_ids)
    weighted = (route_weight[:, :, None] * out_grad.astype(jnp.float32)[:, None, :]).astype(jnp.bfloat16).reshape(2 * TOKENS, D)
    routed = jnp.zeros((EXPERTS * SLOTS, D), jnp.bfloat16).at[rows].set(weighted).reshape(EXPERTS, SLOTS, D)
    gate_grad, up_grad, down_grad, back = lax.map(expert_step, (expert_inputs, routed, gate_weight, up_weight, down_weight))
    pair_back = back.reshape(EXPERTS * SLOTS, D)[rows].astype(jnp.float32).reshape(TOKENS, 2, D)
    resid_grad = (out_grad.astype(jnp.float32) + pair_back[:, 0] + pair_back[:, 1]).astype(jnp.bfloat16)
    gate_vals = out_gate.astype(jnp.float32)
    conv_vals = conv_out.astype(jnp.float32)
    mixed_in = (gate_vals * conv_vals).astype(jnp.bfloat16)
    proj_grad = jnp.dot(resid_grad.T, mixed_in, preferred_element_type=jnp.float32) * (1.0 / math.sqrt(TOKENS))
    mix_grad = jnp.dot(resid_grad, proj_weight, preferred_element_type=jnp.float32)
    out_gate_grad = (mix_grad * conv_vals).astype(jnp.bfloat16)
    conv_grad = lax.optimization_barrier((mix_grad * gate_vals).astype(jnp.bfloat16)).astype(jnp.float32)
    padded = jnp.pad(conv_grad, ((1, 1), (0, 0)))
    tap_vals = conv_taps.astype(jnp.float32)
    value_grad = padded[2:] * tap_vals[0] + padded[1:-1] * tap_vals[1] + padded[:-2] * tap_vals[2]
    in_gate_grad = (value_grad * values.astype(jnp.float32)).astype(jnp.bfloat16)
    values_grad = (value_grad * in_gate.astype(jnp.float32)).astype(jnp.bfloat16)
    return (resid_grad, out_gate_grad, in_gate_grad, values_grad, proj_grad, gate_grad, up_grad, down_grad)
```

```python
import math

import jax
import jax.numpy as jnp
from jax import lax
from jax.experimental import pallas as pl
from jax.experimental.pallas import tpu as pltpu
from jax.sharding import PartitionSpec as P


BF = jnp.bfloat16
F32 = jnp.float32


def swap(x, axis, mask):
    devices = lax.axis_size(axis)
    return lax.ppermute(x, axis, [(i, i ^ mask) for i in range(devices)])


def dot(left, right, dims):
    return lax.dot_general(left, right, (dims, ((), ())), preferred_element_type=F32)


def contract_first(left, right):
    return dot(left, right, ((0,), (0,)))


def contract_last(left, right):
    return dot(left, right, ((1,), (1,)))


def place_rows(pieces, height, index=None):
    sources = [(p, r) for p, x in enumerate(pieces) for r in range(x.shape[0] // height)]
    width, count = pieces[0].shape[1], len(sources)
    if index is None:
        index = jnp.zeros((), jnp.int32)

    def body(idx_ref, *refs):
        out, sems = refs[len(pieces)], refs[len(pieces) + 1]
        copies = []
        for n, (p, r) in enumerate(sources):
            place = pl.multiple_of((idx_ref[0] ^ n) * height, height)
            copies.append(
                pltpu.make_async_copy(
                    refs[p].at[pl.ds(r * height, height)],
                    out.at[pl.ds(place, height)],
                    sems.at[n],
                )
            )
        for copy in copies:
            copy.start()
        for copy in copies:
            copy.wait()

    return pl.pallas_call(
        body,
        in_specs=[pl.BlockSpec(memory_space=pltpu.SMEM)]
        + [pl.BlockSpec(memory_space=pl.ANY)] * len(pieces),
        out_specs=pl.BlockSpec(memory_space=pltpu.VMEM),
        out_shape=jax.ShapeDtypeStruct((count * height, width), pieces[0].dtype),
        scratch_shapes=[pltpu.SemaphoreType.DMA((count,))],
    )(index.reshape(1), *pieces)


def gather_tp(x, t, devices):
    step = devices // 2
    mask = step
    pieces = {0: x}
    while mask:
        for have in list(pieces):
            pieces[have ^ mask] = swap(pieces[have], "tp", mask)
        mask //= 2
    return order_blocks([pieces[m] for m in range(devices)], t)


def order_blocks(pieces, t):
    count = len(pieces)
    mask = 1
    while mask < count:
        flip = (t & mask) != 0
        pieces = [jnp.where(flip, pieces[m ^ mask], pieces[m]) for m in range(count)]
        mask *= 2
    return jnp.concatenate(pieces, axis=1)


def weight_rows(weight, t, m, devices):
    rows = weight.shape[0] // devices
    return lax.dynamic_slice_in_dim(weight, (t ^ m) * rows, rows, axis=0)


def scatter_tp(part, devices):
    held = {m: part(m) for m in range(devices - 1, -1, -1)}
    mask, first = 1, None
    while mask < devices:
        keep = [m for m in held if not m & mask]
        for m in keep:
            got = swap(held[m ^ mask].astype(BF), "tp", mask)
            first = got if first is None else first
            held[m] = held[m] + got.astype(F32)
        held = {m: held[m] for m in keep}
        mask *= 2
    return held[0].astype(BF), first


def per_device(
    out_grad,
    route_ids,
    route_weight,
    expert_inputs,
    gate_weight,
    up_weight,
    down_weight,
    out_gate,
    in_gate,
    values,
    conv_out,
    conv_taps,
    proj_weight,
):
    n_sp = lax.axis_size("sp")
    n_tp = lax.axis_size("tp")
    sp = lax.axis_index("sp").astype(jnp.int32)
    t = lax.axis_index("tp").astype(jnp.int32)
    tok_rows = out_grad.shape[0]
    capacity = 4 * tok_rows // n_sp
    half = n_sp // 2
    inputs, gate_w, up_w, down_w = (
        expert_inputs[0],
        gate_weight[0],
        up_weight[0],
        down_weight[0],
    )

    experts = jnp.arange(n_sp, dtype=jnp.int32)[None, :]
    hot = [(route_ids[:, k : k + 1] == experts).astype(F32) for k in range(2)]
    before = (
        jnp.arange(tok_rows)[:, None] > jnp.arange(tok_rows)[None, :]
    ).astype(BF)
    earlier = jnp.dot(before, (hot[0] + hot[1]).astype(BF), preferred_element_type=F32)
    slots = [
        (route_ids[:, k] ^ sp) * capacity
        + jnp.sum(earlier * hot[k], axis=1).astype(jnp.int32)
        for k in range(2)
    ]
    positions = jnp.arange(n_sp * capacity, dtype=jnp.int32)[:, None]
    chosen = [positions == slots[k][None, :] for k in range(2)]
    dispatch = jnp.concatenate([c.astype(BF) for c in chosen], axis=1)
    combiner = (chosen[0] | chosen[1]).astype(BF)
    grad32 = out_grad.astype(F32)
    weighted = jnp.concatenate(
        [(route_weight[:, k : k + 1] * grad32).astype(BF) for k in range(2)], axis=0
    )
    outgoing = jnp.dot(dispatch, weighted, preferred_element_type=F32).astype(BF)

    def block(x, s):
        return x[s * capacity : (s + 1) * capacity]

    arrived = {}
    for s in range(n_sp - 1, -1, -1):
        arrived[s] = block(outgoing, s) if s == 0 else swap(block(outgoing, s), "sp", s)

    inputs = place_rows([inputs], capacity, sp)
    pre_gate = jnp.dot(inputs, gate_w, preferred_element_type=F32)
    pre_up = jnp.dot(inputs, up_w, preferred_element_type=F32)
    sigmoid_g = jax.nn.sigmoid(pre_gate)
    activated = pre_gate * sigmoid_g
    hidden = (activated * pre_up).astype(BF)
    slope = pre_up * sigmoid_g * (1.0 + pre_gate * (1.0 - sigmoid_g))
    hidden, slope, activated = lax.optimization_barrier((hidden, slope, activated))

    gate_vals = out_gate.astype(F32)
    conv_vals = conv_out.astype(F32)
    mixed_in = (gate_vals * conv_vals).astype(BF)

    mixed_late, _ = lax.optimization_barrier((mixed_in, arrived[1]))
    pair = jnp.concatenate([mixed_late, swap(mixed_late, "sp", 1)], axis=0)
    mixed_pieces = [pair] + [swap(pair, "sp", s) for s in range(2, n_sp, 2)]

    rows = half * capacity
    returned = {}
    routed_list, d_gate_list, d_up_list = {}, {}, {}
    for part_at in (1, 0):
        lower = part_at * rows
        local = place_rows(
            [arrived[s] for s in range(part_at * half, (part_at + 1) * half)], capacity
        )
        routed = gather_tp(local, t, n_tp)
        if part_at == 0:
            routed, _ = lax.optimization_barrier((routed, d_gate_list[1]))
        else:
            routed = lax.optimization_barrier(routed)
        d_hidden = contract_last(routed, down_w)
        d_gate = (d_hidden * slope[lower : lower + rows]).astype(BF)
        d_up = (d_hidden * activated[lower : lower + rows]).astype(BF)
        d_gate, d_up = lax.optimization_barrier((d_gate, d_up))
        routed_list[part_at], d_gate_list[part_at], d_up_list[part_at] = routed, d_gate, d_up

        def part(m):
            return contract_last(d_gate, weight_rows(gate_w, t, m, n_tp)) + contract_last(
                d_up, weight_rows(up_w, t, m, n_tp)
            )

        summed, first = scatter_tp(part, n_tp)
        if part_at == 1:
            first_far = first
        if part_at == 0:
            summed, mixed_pieces = lax.optimization_barrier((summed, mixed_pieces))
        for s in range((part_at + 1) * half - 1, part_at * half - 1, -1):
            piece = block(summed, s - part_at * half)
            returned[s] = piece if s == 0 else swap(piece, "sp", s)

    routed = jnp.concatenate([routed_list[0], routed_list[1]])
    d_gate = jnp.concatenate([d_gate_list[0], d_gate_list[1]])
    d_up = jnp.concatenate([d_up_list[0], d_up_list[1]])
    routed, d_gate, d_up, _ = lax.optimization_barrier((routed, d_gate, d_up, first_far))
    slot_scale = 1.0 / math.sqrt(expert_inputs.shape[1])
    gate_grad = (contract_first(inputs, d_gate) * slot_scale).astype(BF)[None]
    up_grad = (contract_first(inputs, d_up) * slot_scale).astype(BF)[None]
    down_grad = (contract_first(hidden, routed) * slot_scale).astype(BF)[None]

    mixed_all = place_rows(mixed_pieces, tok_rows, sp)

    moe_part = contract_first(
        combiner, place_rows([returned[s] for s in range(n_sp)], capacity)
    )
    resid_grad = (grad32 + moe_part).astype(BF)
    resid_full = lax.all_gather(resid_grad, "tp", axis=1, tiled=True)
    mix_grad = jnp.dot(resid_full, proj_weight, preferred_element_type=F32)
    out_gate_grad = (mix_grad * conv_vals).astype(BF)
    conv_grad = (mix_grad * gate_vals).astype(BF)
    up = [(i, i + 1) for i in range(n_sp - 1)]
    down = [(i + 1, i) for i in range(n_sp - 1)]
    prev_row = lax.ppermute(conv_grad[-1:], "sp", up)
    next_row = lax.ppermute(conv_grad[:1], "sp", down)
    padded = jnp.concatenate([prev_row, conv_grad, next_row], axis=0).astype(F32)
    tap_vals = conv_taps.astype(F32)
    value_grad = padded[2:] * tap_vals[0] + padded[1:-1] * tap_vals[1] + padded[:-2] * tap_vals[2]
    in_gate_grad = (value_grad * values.astype(F32)).astype(BF)
    values_grad = (value_grad * in_gate.astype(F32)).astype(BF)

    share = tok_rows // n_tp
    width = resid_full.shape[1] // n_sp
    token_scale = 1.0 / math.sqrt(tok_rows * n_sp)
    mine = lax.dynamic_slice_in_dim(resid_full, t * share, share, axis=0)
    by_owner = mine.reshape(share, n_sp, width).transpose(1, 0, 2)
    owned = lax.all_to_all(by_owner, "sp", split_axis=0, concat_axis=0, tiled=True)
    owned = owned.reshape(n_sp * share, width)
    columns = lax.all_gather(owned, "tp", axis=0, tiled=True)
    columns = (
        columns.reshape(n_tp, n_sp, share, width)
        .transpose(1, 0, 2, 3)
        .reshape(n_sp * tok_rows, width)
    )
    proj_grad = contract_first(columns, mixed_all) * token_scale
    return (
        resid_grad,
        out_gate_grad,
        in_gate_grad,
        values_grad,
        proj_grad,
        gate_grad,
        up_grad,
        down_grad,
    )


def solution(mesh):
    in_specs = (
        P("sp", "tp"),
        P("sp", None),
        P("sp", None),
        P("sp", None, None),
        P("sp", None, "tp"),
        P("sp", None, "tp"),
        P("sp", "tp", None),
        P("sp", "tp"),
        P("sp", "tp"),
        P("sp", "tp"),
        P("sp", "tp"),
        P(None, "tp"),
        P(None, "tp"),
    )
    out_specs = (
        P("sp", "tp"),
        P("sp", "tp"),
        P("sp", "tp"),
        P("sp", "tp"),
        P("sp", "tp"),
        P("sp", None, "tp"),
        P("sp", None, "tp"),
        P("sp", "tp", None),
    )
    return jax.shard_map(
        per_device, mesh=mesh, in_specs=in_specs, out_specs=out_specs, check_vma=False
    )
```
